32 devices in a mesh: ep: 32 (over z, y, x, core).
Axes of the slice: x: 2, y: 2, z: 4, core: 2. Of those that a mesh axis runs over, the one named last changes fastest.
Arguments:
- tokens: bfloat16 [128, 2048], P('ep'), may hold values from -6 to 6
- recurrent_state: float32 [128, 8, 128, 128], P('ep'), may hold values from -4 to 4
- query_weight: bfloat16 [2048, 1024], P(None, 'ep'), may hold values from -0.125 to 0.125
- forget_weight: bfloat16 [2048, 1024], P(None, 'ep'), may hold values from -0.125 to 0.125
- input_weight: bfloat16 [2048, 1024], P(None, 'ep'), may hold values from -0.125 to 0.125
- outgate_weight: bfloat16 [2048, 1024], P(None, 'ep'), may hold values from -0.125 to 0.125
- lower_bound: float32 [1024], replicated, may hold values from 0 to 0.9
- head_gain: float32 [128], replicated, may hold values from 0.1 to 1.9
- mixout_weight: bfloat16 [1024, 2048], P(None, 'ep'), may hold values from -0.1875 to 0.1875
- first_gain: float32 [2048], replicated, may hold values from 0.1 to 1.9
- first_bias: float32 [2048], replicated, may hold values from -1.5 to 1.5
- router_weight: bfloat16 [2048, 8], replicated, may hold values from -0.125 to 0.125
- branch_vector: bfloat16 [2048], replicated, may hold values from -0.125 to 0.125
- dense_gate_weight: bfloat16 [2048, 5632], P(None, 'ep'), may hold values from -0.125 to 0.125
- dense_up_weight: bfloat16 [2048, 5632], P(None, 'ep'), may hold values from -0.125 to 0.125
- dense_down_weight: bfloat16 [5632, 2048], P('ep'), may hold values from -0.078125 to 0.078125
- expert_gate_weight: bfloat16 [2048, 57344], P(None, 'ep'), may hold values from -0.125 to 0.125
- expert_up_weight: bfloat16 [2048, 57344], P(None, 'ep'), may hold values from -0.125 to 0.125
- expert_down_weight: bfloat16 [57344, 2048], P('ep'), may hold values from -0.0625 to 0.0625
- second_gain: float32 [2048], replicated, may hold values from 0.1 to 1.9
- second_bias: float32 [2048], replicated, may hold values from -1.5 to 1.5
- routes: int32 [128, 2], replicated, may hold values from 0 to 7, all different within a row; in each aligned block of 4 rows (0 to 3, 4 to 7, ...) at most 2 rows name the same one
Outputs:
- output: bfloat16 [128, 2048], P('ep')
- new_state: float32 [128, 8, 128, 128], P('ep')
The draws below stay inside these ranges and needn't reach their ends.
Inputs may be any that keep to these rules, and one draw needn't show every extreme that they name: `routes`: each row names two different experts; in the rows of one device no expert is named more than 2 times, a bound that some block reaches in some device's rows.
All inputs are finite; a program needn't handle non-finite values.
Results may differ from the reference program's by a relative error of at most 0.0095.
Values may be sent and summed in bfloat16 or wider, within the bound.
A program may use at most 64 MiB of HBM per device.

```python
import math
import jax
import jax.numpy as jnp
import numpy as np
from jax import lax

D = 2048
HGW = 1024
DK = 128
HEADS = 8
EXPERTS = 8
FF_E = 7168
FD = 5632
B_DEV = 4
CAP = 2
TOKENS = 128
N_EP = 32


def block_scale(rng, extent, cuts, least, high):
    level, own = 1.0, jax.random.fold_in(rng, 6)
    for axis_at, blocks in cuts:
        draws = jnp.exp(jax.random.uniform(jax.random.fold_in(own, axis_at), (blocks,), jnp.float32, least / len(cuts), high / len(cuts)))
        level = level * jnp.repeat(draws, extent[axis_at] // blocks).reshape([-1 if axis == axis_at else 1 for axis in range(len(extent))])
    return level


def deal_out(key, own, number, rows, amount, top, reach, skew):
    order = jax.random.permutation(key, amount)
    crowded, usual = portions_of(amount, rows * top, reach, skew, True), portions_of(amount, rows * top, reach, skew, False)
    places = jnp.arange(amount)

    def named(sizes, rotation):
        used = int((sizes > 0).sum())
        fixed = max(1, used // 4)
        moved = fixed + (places - fixed + rotation * (used - fixed)) % max(1, amount - fixed)
        return jnp.zeros((amount,), jnp.int32).at[order[jnp.where(places < fixed, places, moved)]].set(jnp.asarray(sizes, jnp.int32))

    sizes = jnp.where(number % 4 == 0, named(crowded, number // 4), named(usual, number - number // 4 - 1))
    mixed = jax.random.permutation(jax.random.fold_in(own, 3), amount)
    donor, sink = mixed[0:amount // 2 * 2:2], mixed[1:amount // 2 * 2:2]
    room = jnp.minimum(sizes[donor] - 1, reach - sizes[sink]) // 2
    room = jnp.where((donor == order[0]) | (sink == order[0]) | (sizes[sink] == 0), 0, jnp.maximum(room, 0))
    moved = jax.random.randint(jax.random.fold_in(own, 4), (amount // 2,), 0, 1 << 20) % (room + 1)
    sizes = sizes.at[donor].add(-moved).at[sink].add(moved)
    members = jnp.searchsorted(jnp.cumsum(sizes), jnp.arange(rows * top), side="right").astype(jnp.int32)
    table = members.reshape(top, rows).T
    table = table[jax.random.permutation(jax.random.fold_in(own, 1), rows)]
    rotation = jax.random.randint(jax.random.fold_in(own, 2), (rows, 1), 0, top)
    return jnp.take_along_axis(table, (jnp.arange(top)[None, :] + rotation) % top, axis=1)


def portions_of(amount, total, reach, slope, full):
    weights = [(1 << 20) // math.isqrt(rank ** slope) + 1 for rank in range(1, amount + 1)]
    largest = reach if full else min(reach, max(-(-total // amount), total * weights[0] // sum(weights)))
    least = 1 if total - largest >= amount - 1 else 0
    holding, spare = [largest] + [least] * (amount - 1), total - largest - least * (amount - 1)
    while spare > 0:
        free = [i for i in range(1, amount) if holding[i] < largest] or [i for i in range(1, amount) if holding[i] < reach]
        mass, remaining = sum([weights[i] for i in free]), spare
        for i in free:
            addition = min(reach - holding[i], max(1, remaining * weights[i] // mass), spare)
            holding[i] = holding[i] + addition
            spare = spare - addition
    return np.array(holding)


def bell_draw(stream_key, shape, scale, limit, pieces=(), kind=jnp.bfloat16):
    level = block_scale(stream_key, shape, pieces, -0.22, 0.18) if pieces else 1.0
    result = jax.random.normal(stream_key, shape, jnp.float32) * scale * level
    return jnp.minimum(jnp.maximum(result, -limit), limit).astype(kind)


def setup_inputs(seed: int = 0) -> dict:
    keys = jax.random.split(jax.random.key(seed), 23)
    tokens = bell_draw(keys[0], (TOKENS, D), 1.0, 6.0, ((0, 32),))
    recurrent_state = bell_draw(keys[1], (TOKENS, HEADS, DK, DK), 0.5, 4.0, ((0, 32),), jnp.float32)
    query_weight = bell_draw(keys[2], (D, HGW), D ** -0.5, 0.125, ((1, 32),))
    forget_weight = bell_draw(keys[3], (D, HGW), D ** -0.5, 0.125, ((1, 32),))
    input_weight = bell_draw(keys[4], (D, HGW), D ** -0.5, 0.125, ((1, 32),))
    outgate_weight = bell_draw(keys[5], (D, HGW), D ** -0.5, 0.125, ((1, 32),))
    lower_bound = jnp.clip(jax.random.uniform(keys[6], (HGW,), jnp.float32, 0.0, 0.9), 0.0, 0.9)
    head_gain = jnp.clip(1.0 + 0.18 * jax.random.normal(keys[7], (DK,), jnp.float32), 0.1, 1.9)
    mixout_weight = bell_draw(keys[8], (HGW, D), HGW ** -0.5, 0.1875, ((1, 32),))
    first_gain = jnp.clip(1.0 + 0.18 * jax.random.normal(keys[9], (D,), jnp.float32), 0.1, 1.9)
    first_bias = bell_draw(keys[10], (D,), 0.3, 1.5, (), jnp.float32)
    router_weight = bell_draw(keys[11], (D, EXPERTS), D ** -0.5, 0.125)
    branch_vector = bell_draw(keys[12], (D,), D ** -0.5, 0.125)
    dense_gate_weight = bell_draw(keys[13], (D, FD), D ** -0.5, 0.125, ((1, 32),))
    dense_up_weight = bell_draw(keys[14], (D, FD), D ** -0.5, 0.125, ((1, 32),))
    dense_down_weight = bell_draw(keys[15], (FD, D), FD ** -0.5, 0.078125, ((0, 32),))
    expert_gate_weight = bell_draw(keys[16], (D, EXPERTS * FF_E), D ** -0.5, 0.125, ((1, 32),))
    expert_up_weight = bell_draw(keys[17], (D, EXPERTS * FF_E), D ** -0.5, 0.125, ((1, 32),))
    expert_down_weight = bell_draw(keys[18], (EXPERTS * FF_E, D), FF_E ** -0.5, 0.0625, ((0, 32),))
    second_gain = jnp.clip(1.0 + 0.18 * jax.random.normal(keys[19], (D,), jnp.float32), 0.1, 1.9)
    second_bias = bell_draw(keys[20], (D,), 0.3, 1.5, (), jnp.float32)
    routes_keys = jax.random.split(jax.random.fold_in(keys[21], 1), TOKENS // B_DEV)
    routes_turns = jax.random.permutation(jax.random.fold_in(keys[21], 3), TOKENS // B_DEV)
    routes = jax.vmap(lambda own, number: deal_out(jax.random.fold_in(keys[21], 2), own, number, B_DEV, EXPERTS, 2, CAP, 2))(routes_keys, routes_turns).reshape((TOKENS, 2))
    return dict(tokens=tokens, recurrent_state=recurrent_state, query_weight=query_weight, forget_weight=forget_weight, input_weight=input_weight, outgate_weight=outgate_weight, lower_bound=lower_bound, head_gain=head_gain, mixout_weight=mixout_weight, first_gain=first_gain, first_bias=first_bias, router_weight=router_weight, branch_vector=branch_vector, dense_gate_weight=dense_gate_weight, dense_up_weight=dense_up_weight, dense_down_weight=dense_down_weight, expert_gate_weight=expert_gate_weight, expert_up_weight=expert_up_weight, expert_down_weight=expert_down_weight, second_gain=second_gain, second_bias=second_bias, routes=routes)


ALPHA = 8.0 ** 0.25
NORM_EPS = 1e-05
HEAD_EPS = 1e-06

def layer_norm(mixture, gain, bias):
    center = lax.optimization_barrier(jnp.mean(mixture, axis=-1, keepdims=True))
    spread = lax.optimization_barrier(jnp.mean(jnp.square(mixture - center), axis=-1, keepdims=True))
    return (mixture - center) * lax.rsqrt(spread + NORM_EPS) * gain + bias

def recurrence(projected, state, lower_bound, head_gain):
    nseq, heads, width = (state.shape[0], state.shape[1], state.shape[2])
    query = projected[:, 0].astype(jnp.float32).reshape(nseq, heads, width)
    forget_in = projected[:, 1].astype(jnp.float32)
    value = projected[:, 2].astype(jnp.float32).reshape(nseq, heads, width)
    outgate = projected[:, 3].astype(jnp.float32)
    forget = (lower_bound + (1.0 - lower_bound) * jax.nn.sigmoid(forget_in)).reshape(nseq, heads, width)
    keyed = ((1.0 - lower_bound) * jax.nn.sigmoid(-forget_in)).reshape(nseq, heads, width)
    fresh = forget[..., None] * state + keyed[..., None] * value[:, :, None, :]
    read = jnp.einsum('bhkv,bhk->bhv', fresh, query, precision=lax.Precision.HIGHEST)
    scaled = read * lax.rsqrt(lax.optimization_barrier(jnp.mean(jnp.square(read), axis=-1, keepdims=True)) + HEAD_EPS) * head_gain
    mixed = (scaled.reshape(nseq, heads * width) * jax.nn.silu(outgate)).astype(jnp.bfloat16)
    return (mixed, fresh)

def reference(tokens, recurrent_state, query_weight, forget_weight, input_weight, outgate_weight, lower_bound, head_gain, mixout_weight, first_gain, first_bias, router_weight, branch_vector, dense_gate_weight, dense_up_weight, dense_down_weight, expert_gate_weight, expert_up_weight, expert_down_weight, second_gain, second_bias, routes):
    f32 = jnp.float32
    parts = [jnp.dot(tokens, weight, preferred_element_type=f32).astype(jnp.bfloat16) for weight in (query_weight, forget_weight, input_weight, outgate_weight)]
    projected = jnp.stack(parts, axis=1)
    mixed, new_state = recurrence(projected, recurrent_state, lower_bound, head_gain)
    mix_out = jnp.dot(mixed, mixout_weight, preferred_element_type=f32).astype(jnp.bfloat16)
    normed = layer_norm(ALPHA * tokens.astype(f32) + mix_out.astype(f32), first_gain, first_bias).astype(jnp.bfloat16)
    width = normed.shape[1]
    logits = jnp.dot(normed, router_weight, preferred_element_type=f32)
    expert_ids = jnp.arange(EXPERTS, dtype=jnp.int32)
    first_pick = routes[:, 0]
    second_pick = routes[:, 1]
    first_logit = lax.optimization_barrier(jnp.sum(jnp.where(first_pick[:, None] == expert_ids[None, :], logits, 0.0), axis=1))
    second_logit = lax.optimization_barrier(jnp.sum(jnp.where(second_pick[:, None] == expert_ids[None, :], logits, 0.0), axis=1))
    share = jax.nn.sigmoid(first_logit - second_logit)
    branch_gate = jax.nn.sigmoid(jnp.dot(normed, branch_vector, preferred_element_type=f32))
    dense_hidden = (jax.nn.silu(jnp.dot(normed, dense_gate_weight, preferred_element_type=f32)) * jnp.dot(normed, dense_up_weight, preferred_element_type=f32)).astype(jnp.bfloat16)
    channel = branch_gate[:, None] * jnp.dot(dense_hidden, dense_down_weight, preferred_element_type=f32)
    blocks = normed.reshape(N_EP, B_DEV, width).astype(f32)
    slot_ids = jnp.arange(CAP, dtype=jnp.int32)
    for expert in range(EXPERTS):
        on_first = first_pick == expert
        on_second = second_pick == expert
        token_weight = share * on_first.astype(f32) + (1.0 - share) * on_second.astype(f32)
        hits = (on_first | on_second).astype(jnp.int32).reshape(N_EP, B_DEV)
        ranks = jnp.cumsum(hits, axis=1) - 1
        select = ((ranks[:, None, :] == slot_ids[None, :, None]) & (hits[:, None, :] > 0)).astype(f32)
        slot_rows = jnp.einsum('sci,sid->scd', select, blocks, precision=lax.Precision.HIGHEST)
        slot_rows = slot_rows.astype(jnp.bfloat16).reshape(N_EP * CAP, width)
        low = expert * FF_E
        gate_part = jnp.dot(slot_rows, expert_gate_weight[:, low:low + FF_E], preferred_element_type=f32)
        up_part = jnp.dot(slot_rows, expert_up_weight[:, low:low + FF_E], preferred_element_type=f32)
        hidden = (jax.nn.silu(gate_part) * up_part).astype(jnp.bfloat16)
        slot_out = jnp.dot(hidden, expert_down_weight[low:low + FF_E, :], preferred_element_type=f32)
        slot_out = slot_out.reshape(N_EP, CAP, width)
        back = jnp.einsum('sci,scd->sid', select, slot_out, precision=lax.Precision.HIGHEST)
        channel = channel + back.reshape(N_EP * B_DEV, width) * token_weight[:, None]
    output = layer_norm(ALPHA * normed.astype(f32) + channel, second_gain, second_bias).astype(jnp.bfloat16)
    return (output, new_state)
```

```python
import jax
import jax.numpy as jnp
from jax import lax
from jax.sharding import PartitionSpec as P

EXPERTS = 8


ALPHA = 8.0**0.25
NORM_EPS = 1e-05
HEAD_EPS = 1e-06


def layer_norm(mixture, gain, bias):
    center = jnp.mean(mixture, axis=-1, keepdims=True)
    spread = jnp.mean(jnp.square(mixture - center), axis=-1, keepdims=True)
    return (mixture - center) * lax.rsqrt(spread + NORM_EPS) * gain + bias


def recurrence(projected, state, lower_bound, head_gain):
    nseq, heads, width = (state.shape[0], state.shape[1], state.shape[2])
    query = projected[:, 0].astype(jnp.float32).reshape(nseq, heads, width)
    forget_in = projected[:, 1].astype(jnp.float32)
    value = projected[:, 2].astype(jnp.float32).reshape(nseq, heads, width)
    outgate = projected[:, 3].astype(jnp.float32)
    forget = (lower_bound + (1.0 - lower_bound) * jax.nn.sigmoid(forget_in)).reshape(
        nseq, heads, width
    )
    keyed = ((1.0 - lower_bound) * jax.nn.sigmoid(-forget_in)).reshape(nseq, heads, width)
    fresh = forget[..., None] * state + keyed[..., None] * value[:, :, None, :]
    read = jnp.einsum("bhkv,bhk->bhv", fresh, query, precision=lax.Precision.HIGHEST)
    scaled = (
        read * lax.rsqrt(jnp.mean(jnp.square(read), axis=-1, keepdims=True) + HEAD_EPS) * head_gain
    )
    mixed = (scaled.reshape(nseq, heads * width) * jax.nn.silu(outgate)).astype(jnp.bfloat16)
    return (mixed, fresh)


def route_share(rows, picks, router_weight):
    f32 = jnp.float32
    logits = jnp.dot(rows, router_weight, preferred_element_type=f32)
    expert_ids = jnp.arange(EXPERTS, dtype=jnp.int32)
    first_logit = jnp.sum(jnp.where(picks[:, 0:1] == expert_ids[None, :], logits, 0.0), axis=1)
    second_logit = jnp.sum(jnp.where(picks[:, 1:2] == expert_ids[None, :], logits, 0.0), axis=1)
    return jax.nn.sigmoid(first_logit - second_logit)


def spread(block):
    count = lax.axis_size("ep")
    copies = jnp.broadcast_to(block[None], (count,) + block.shape)
    arrived = lax.all_to_all(copies, "ep", split_axis=0, concat_axis=0, tiled=True)
    return arrived.reshape(count * block.shape[0], block.shape[1])


def channel_partial(
    rows,
    routes,
    router_weight,
    branch_vector,
    dense_gate_weight,
    dense_up_weight,
    dense_down_weight,
    expert_gate_weight,
    expert_up_weight,
    expert_down_weight,
):
    f32 = jnp.float32
    share = route_share(rows, routes, router_weight)
    expert = lax.axis_index("ep") // (lax.axis_size("ep") // EXPERTS)
    on_first = routes[:, 0] == expert
    on_second = routes[:, 1] == expert
    weight = jnp.where(on_first, share, jnp.where(on_second, 1.0 - share, 0.0))
    branch_gate = jax.nn.sigmoid(jnp.dot(rows, branch_vector, preferred_element_type=f32))

    def ffn(gate_weight, up_weight, down_weight):
        gate_part = jnp.dot(rows, gate_weight, preferred_element_type=f32)
        up_part = jnp.dot(rows, up_weight, preferred_element_type=f32)
        hidden = (jax.nn.silu(gate_part) * up_part).astype(jnp.bfloat16)
        return jnp.dot(hidden, down_weight, preferred_element_type=f32)

    dense = ffn(dense_gate_weight, dense_up_weight, dense_down_weight)
    routed = ffn(expert_gate_weight, expert_up_weight, expert_down_weight)
    picked = (on_first | on_second)[:, None]
    return branch_gate[:, None] * dense + jnp.where(picked, weight[:, None] * routed, 0.0)


def per_device(
    tokens,
    recurrent_state,
    query_weight,
    forget_weight,
    input_weight,
    outgate_weight,
    lower_bound,
    head_gain,
    mixout_weight,
    first_gain,
    first_bias,
    router_weight,
    branch_vector,
    dense_gate_weight,
    dense_up_weight,
    dense_down_weight,
    expert_gate_weight,
    expert_up_weight,
    expert_down_weight,
    second_gain,
    second_bias,
    routes,
):
    f32 = jnp.float32
    devices = lax.axis_size("ep")
    nseq, width = tokens.shape
    own_cols = query_weight.shape[1]
    stacked = jnp.concatenate([query_weight, forget_weight, input_weight, outgate_weight], axis=1)
    weights = (
        router_weight,
        branch_vector,
        dense_gate_weight,
        dense_up_weight,
        dense_down_weight,
        expert_gate_weight,
        expert_up_weight,
        expert_down_weight,
    )
    gathered = jnp.dot(
        spread(tokens), stacked, preferred_element_type=f32
    ).astype(jnp.bfloat16)
    owned = lax.all_to_all(gathered, "ep", split_axis=0, concat_axis=1, tiled=True)
    projected = (
        owned.reshape(nseq, devices, 4, own_cols)
        .transpose(0, 2, 1, 3)
        .reshape(nseq, 4, devices * own_cols)
    )
    mixed, new_state = recurrence(projected, recurrent_state, lower_bound, head_gain)
    mix_cols = jnp.dot(
        spread(mixed), mixout_weight, preferred_element_type=f32
    ).astype(jnp.bfloat16)
    mix_out = lax.all_to_all(mix_cols, "ep", split_axis=0, concat_axis=1, tiled=True)
    normed = layer_norm(
        ALPHA * tokens.astype(f32) + mix_out.astype(f32), first_gain, first_bias
    ).astype(jnp.bfloat16)
    partial = channel_partial(spread(normed), routes, *weights).astype(jnp.bfloat16)
    arrived = lax.all_to_all(
        partial.reshape(devices, nseq, width), "ep", split_axis=0, concat_axis=0, tiled=True
    )
    channel = jnp.sum(arrived.astype(f32), axis=0)
    output = layer_norm(ALPHA * normed.astype(f32) + channel, second_gain, second_bias).astype(
        jnp.bfloat16
    )
    return (output, new_state)


def solution(mesh):
    return jax.shard_map(
        per_device,
        mesh=mesh,
        in_specs=(
            P("ep", None),
            P("ep", None, None, None),
            P(None, "ep"),
            P(None, "ep"),
            P(None, "ep"),
            P(None, "ep"),
            P(),
            P(),
            P(None, "ep"),
            P(),
            P(),
            P(),
            P(),
            P(None, "ep"),
            P(None, "ep"),
            P("ep", None),
            P(None, "ep"),
            P(None, "ep"),
            P("ep", None),
            P(),
            P(),
            P(),
        ),
        out_specs=(P("ep", None), P("ep", None, None, None)),
        check_vma=False,
    )
```

```python
import jax
import jax.numpy as jnp
from jax import lax
import functools

from jax.experimental import pallas as pl
from jax.experimental.pallas import tpu as pltpu
from jax.sharding import PartitionSpec as P

EXPERTS = 8
MESH = pl.DeviceIdType.MESH


ALPHA = 8.0**0.25
NORM_EPS = 1e-05
HEAD_EPS = 1e-06


def layer_norm(mixture, gain, bias):
    center = jnp.mean(mixture, axis=-1, keepdims=True)
    spread = jnp.mean(jnp.square(mixture - center), axis=-1, keepdims=True)
    return (mixture - center) * lax.rsqrt(spread + NORM_EPS) * gain + bias


def recurrence(projected, state, lower_bound, head_gain):
    nseq, heads, width = (state.shape[0], state.shape[1], state.shape[2])
    query = projected[:, 0].astype(jnp.float32).reshape(nseq, heads, width)
    forget_in = projected[:, 1].astype(jnp.float32)
    value = projected[:, 2].astype(jnp.float32).reshape(nseq, heads, width)
    outgate = projected[:, 3].astype(jnp.float32)
    forget = (lower_bound + (1.0 - lower_bound) * jax.nn.sigmoid(forget_in)).reshape(
        nseq, heads, width
    )
    keyed = ((1.0 - lower_bound) * jax.nn.sigmoid(-forget_in)).reshape(nseq, heads, width)
    fresh = forget[..., None] * state + keyed[..., None] * value[:, :, None, :]
    read = jnp.einsum("bhkv,bhk->bhv", fresh, query, precision=lax.Precision.HIGHEST)
    scaled = (
        read * lax.rsqrt(jnp.mean(jnp.square(read), axis=-1, keepdims=True) + HEAD_EPS) * head_gain
    )
    mixed = (scaled.reshape(nseq, heads * width) * jax.nn.silu(outgate)).astype(jnp.bfloat16)
    return (mixed, fresh)


def greet(n, me):
    barrier = pltpu.get_barrier_semaphore()

    @pl.loop(1, n)
    def _(k):
        pl.semaphore_signal(
            barrier, inc=1, device_id=(lax.rem(me + k, n),), device_id_type=MESH
        )

    pl.semaphore_wait(barrier, n - 1)


def start_all(source, dest, send_sem, recv_sem, n, me):
    @pl.loop(1, n)
    def _(k):
        peer = lax.rem(me + k, n)
        pltpu.make_async_remote_copy(
            src_ref=source(peer),
            dst_ref=dest.at[me],
            send_sem=send_sem.at[k],
            recv_sem=recv_sem.at[k],
            device_id=(peer,),
            device_id_type=MESH,
        ).start()


def wait_all(source, dest, send_sem, recv_sem, n, me):
    @pl.loop(1, n)
    def _(k):
        peer = lax.rem(me + k, n)
        pltpu.make_async_remote_copy(
            src_ref=source(peer),
            dst_ref=dest.at[lax.rem(me + n - k, n)],
            send_sem=send_sem.at[k],
            recv_sem=recv_sem.at[k],
            device_id=(peer,),
            device_id_type=MESH,
        ).wait()


def flatten_rows(blocks, flat, n, nseq):
    group = max(1, 16 // nseq)

    @pl.loop(0, n // group)
    def _(i):
        parts = [blocks[i * group + j].astype(jnp.float32) for j in range(group)]
        at = pl.multiple_of(i * (group * nseq), group * nseq)
        flat[pl.ds(at, group * nseq), :] = jnp.concatenate(parts, axis=0).astype(flat.dtype)


def split_rows(flat, blocks, n, nseq):
    group = max(1, 8 // nseq)

    @pl.loop(0, n // group)
    def _(i):
        at = pl.multiple_of(i * (group * nseq), group * nseq)
        taken = flat[pl.ds(at, group * nseq), :]
        for j in range(group):
            blocks[i * group + j] = taken[j * nseq : (j + 1) * nseq].astype(blocks.dtype)


def project_kernel(
    n, block_ref, weight_hbm, out_ref,
    weight, gathered, rows, made, outgoing, landed,
    weight_sem, gather_send, gather_recv, back_send, back_recv,
):
    me = lax.axis_index("ep")
    nseq = block_ref.shape[0]
    load = pltpu.make_async_copy(weight_hbm, weight, weight_sem)
    load.start()
    greet(n, me)
    own = lambda peer: block_ref
    start_all(own, gathered, gather_send, gather_recv, n, me)
    gathered[me] = block_ref[...]
    wait_all(own, gathered, gather_send, gather_recv, n, me)
    flatten_rows(gathered, rows, n, nseq)
    load.wait()
    made[...] = jnp.dot(
        rows[...], weight[...], preferred_element_type=jnp.float32
    )
    split_rows(made, outgoing, n, nseq)
    part = lambda peer: outgoing.at[peer]
    start_all(part, landed, back_send, back_recv, n, me)
    landed[me] = outgoing[me]
    wait_all(part, landed, back_send, back_recv, n, me)
    out_ref[...] = landed[...]


def exchange_semaphores(n):
    return [pltpu.SemaphoreType.DMA((n,))] * 4


def project(block, weight, n, collective_id):
    nseq, width = block.shape
    cols = weight.shape[1]
    bf16, f32 = jnp.bfloat16, jnp.float32
    return pl.pallas_call(
        functools.partial(project_kernel, n),
        out_shape=jax.ShapeDtypeStruct((n, nseq, cols), bf16),
        in_specs=[
            pl.BlockSpec(memory_space=pltpu.VMEM),
            pl.BlockSpec(memory_space=pl.ANY),
        ],
        out_specs=pl.BlockSpec(memory_space=pltpu.VMEM),
        scratch_shapes=[
            pltpu.VMEM(weight.shape, bf16),
            pltpu.VMEM((n, nseq, width), bf16),
            pltpu.VMEM((n * nseq, width), bf16),
            pltpu.VMEM((n * nseq, cols), f32),
            pltpu.VMEM((n, nseq, cols), bf16),
            pltpu.VMEM((n, nseq, cols), bf16),
            pltpu.SemaphoreType.DMA,
            *exchange_semaphores(n),
        ],
        compiler_params=pltpu.CompilerParams(
            collective_id=collective_id, has_side_effects=True, vmem_limit_bytes=24 * 2**20
        ),
    )(block, weight)


def column_tile(cols):
    return 256 if cols % 256 == 0 else cols


def for_tiles(cols, body):
    tile = column_tile(cols)
    if tile == cols:
        body(slice(None))
    else:
        pl.loop(0, cols // tile)(lambda i: body(pl.ds(pl.multiple_of(i * tile, tile), tile)))


def channel_kernel(
    n, block_ref, pick_ref, small_ref, gain_ref, bias_ref,
    gate_hbm, up_hbm, down_hbm, dense_gate_hbm, dense_up_hbm, dense_down_hbm, out_ref,
    gate_w, up_w, down_w, dense_gate_w, dense_up_w, dense_down_w,
    gathered, rows, hidden, dense_hidden, made, outgoing, landed,
    weight_sem, gather_send, gather_recv, back_send, back_recv,
):
    f32 = jnp.float32
    me = lax.axis_index("ep")
    nseq, width = block_ref.shape
    pairs = (
        (dense_gate_hbm, dense_gate_w),
        (dense_up_hbm, dense_up_w),
        (gate_hbm, gate_w),
        (up_hbm, up_w),
        (dense_down_hbm, dense_down_w),
        (down_hbm, down_w),
    )
    loads = [
        pltpu.make_async_copy(there, here, weight_sem.at[i]) for i, (there, here) in enumerate(pairs)
    ]
    for load in loads:
        load.start()
    greet(n, me)
    own = lambda peer: block_ref
    start_all(own, gathered, gather_send, gather_recv, n, me)
    gathered[me] = block_ref[...]
    wait_all(own, gathered, gather_send, gather_recv, n, me)
    flatten_rows(gathered, rows, n, nseq)
    dot = functools.partial(jnp.dot, preferred_element_type=f32)

    small = dot(rows[...], small_ref[...])
    picks = pick_ref[...]
    logit_gap = jnp.sum(small[:, :EXPERTS] * picks[:, :EXPERTS], axis=1, keepdims=True)
    share = jax.nn.sigmoid(logit_gap)
    branch_gate = jax.nn.sigmoid(small[:, EXPERTS : EXPERTS + 1])
    on_first = picks[:, EXPERTS : EXPERTS + 1] > 0
    on_second = picks[:, EXPERTS + 1 : EXPERTS + 2] > 0
    weight = jnp.where(on_first, share, jnp.where(on_second, 1.0 - share, 0.0))

    def fill(target, gate, up):
        def body(at):
            gate_part = dot(rows[...], gate[:, at])
            up_part = dot(rows[...], up[:, at])
            target[:, at] = (jax.nn.silu(gate_part) * up_part).astype(jnp.bfloat16)

        for_tiles(target.shape[1], body)

    for load in loads[:2]:
        load.wait()
    fill(dense_hidden, dense_gate_w, dense_up_w)
    for load in loads[2:4]:
        load.wait()
    fill(hidden, gate_w, up_w)
    for load in loads[4:]:
        load.wait()

    def down(at):
        routed = dot(hidden[...], down_w[:, at])
        dense = dot(dense_hidden[...], dense_down_w[:, at])
        made[:, at] = branch_gate * dense + jnp.where(weight > 0, weight * routed, 0.0)

    for_tiles(width, down)
    split_rows(made, outgoing, n, nseq)
    part = lambda peer: outgoing.at[peer]
    start_all(part, landed, back_send, back_recv, n, me)
    landed[me] = outgoing[me]
    wait_all(part, landed, back_send, back_recv, n, me)
    channel = lax.fori_loop(
        0, n, lambda d, total: total + landed[d].astype(f32), jnp.zeros((nseq, width), f32)
    )
    mixture = ALPHA * block_ref[...].astype(f32) + channel
    out_ref[...] = layer_norm(mixture, gain_ref[...], bias_ref[...]).astype(jnp.bfloat16)


def channel_and_norm(
    normed, routes, n, router_weight, branch_vector, dense_gate_weight, dense_up_weight,
    dense_down_weight, expert_gate_weight, expert_up_weight, expert_down_weight, gain, bias,
):
    bf16, f32 = jnp.bfloat16, jnp.float32
    nseq, width = normed.shape
    total = n * nseq
    expert = lax.axis_index("ep") // (n // EXPERTS)
    first = jax.nn.one_hot(routes[:, 0], EXPERTS, dtype=f32)
    second = jax.nn.one_hot(routes[:, 1], EXPERTS, dtype=f32)
    picks = jnp.concatenate([first - second, (routes == expert).astype(f32)], axis=1)
    small = jnp.concatenate([router_weight, branch_vector[:, None]], axis=1)
    weights = (
        expert_gate_weight,
        expert_up_weight,
        expert_down_weight,
        dense_gate_weight,
        dense_up_weight,
        dense_down_weight,
    )
    vmem, anywhere = pl.BlockSpec(memory_space=pltpu.VMEM), pl.BlockSpec(memory_space=pl.ANY)
    return pl.pallas_call(
        functools.partial(channel_kernel, n),
        out_shape=jax.ShapeDtypeStruct((nseq, width), bf16),
        in_specs=[vmem] * 5 + [anywhere] * 6,
        out_specs=vmem,
        scratch_shapes=[
            *[pltpu.VMEM(w.shape, bf16) for w in weights],
            pltpu.VMEM((n, nseq, width), bf16),
            pltpu.VMEM((total, width), bf16),
            pltpu.VMEM((total, expert_gate_weight.shape[1]), bf16),
            pltpu.VMEM((total, dense_gate_weight.shape[1]), bf16),
            pltpu.VMEM((total, width), f32),
            pltpu.VMEM((n, nseq, width), bf16),
            pltpu.VMEM((n, nseq, width), bf16),
            pltpu.SemaphoreType.DMA((6,)),
            *exchange_semaphores(n),
        ],
        compiler_params=pltpu.CompilerParams(
            collective_id=2, has_side_effects=True, vmem_limit_bytes=56 * 2**20
        ),
    )(normed, picks, small, gain[None], bias[None], *weights)


def per_device(
    tokens,
    recurrent_state,
    query_weight,
    forget_weight,
    input_weight,
    outgate_weight,
    lower_bound,
    head_gain,
    mixout_weight,
    first_gain,
    first_bias,
    router_weight,
    branch_vector,
    dense_gate_weight,
    dense_up_weight,
    dense_down_weight,
    expert_gate_weight,
    expert_up_weight,
    expert_down_weight,
    second_gain,
    second_bias,
    routes,
):
    f32 = jnp.float32
    devices = lax.axis_size("ep")
    nseq, width = tokens.shape
    own_cols = query_weight.shape[1]
    stacked = jnp.concatenate([query_weight, forget_weight, input_weight, outgate_weight], axis=1)
    owned = project(tokens, stacked, devices, 0)
    projected = (
        owned.reshape(devices, nseq, 4, own_cols)
        .transpose(1, 2, 0, 3)
        .reshape(nseq, 4, devices * own_cols)
    )
    mixed, new_state = recurrence(projected, recurrent_state, lower_bound, head_gain)
    mix_out = project(mixed, mixout_weight, devices, 1).transpose(1, 0, 2).reshape(nseq, width)
    normed = layer_norm(
        ALPHA * tokens.astype(f32) + mix_out.astype(f32), first_gain, first_bias
    ).astype(jnp.bfloat16)
    output = channel_and_norm(
        normed,
        routes,
        devices,
        router_weight,
        branch_vector,
        dense_gate_weight,
        dense_up_weight,
        dense_down_weight,
        expert_gate_weight,
        expert_up_weight,
        expert_down_weight,
        second_gain,
        second_bias,
    )
    return (output, new_state)


def solution(mesh):
    return jax.shard_map(
        per_device,
        mesh=mesh,
        in_specs=(
            P("ep", None),
            P("ep", None, None, None),
            P(None, "ep"),
            P(None, "ep"),
            P(None, "ep"),
            P(None, "ep"),
            P(),
            P(),
            P(None, "ep"),
            P(),
            P(),
            P(),
            P(),
            P(None, "ep"),
            P(None, "ep"),
            P("ep", None),
            P(None, "ep"),
            P(None, "ep"),
            P("ep", None),
            P(),
            P(),
            P(),
        ),
        out_specs=(P("ep", None), P("ep", None, None, None)),
        check_vma=False,
    )
```

```python
import jax
import jax.numpy as jnp
from jax import lax
import functools

from jax.experimental import pallas as pl
from jax.experimental.pallas import tpu as pltpu
from jax.sharding import PartitionSpec as P

EXPERTS = 8
MESH = pl.DeviceIdType.MESH


ALPHA = 8.0**0.25
NORM_EPS = 1e-05
HEAD_EPS = 1e-06


def layer_norm(mixture, gain, bias):
    center = jnp.mean(mixture, axis=-1, keepdims=True)
    spread = jnp.mean(jnp.square(mixture - center), axis=-1, keepdims=True)
    return (mixture - center) * lax.rsqrt(spread + NORM_EPS) * gain + bias


def recurrence(projected, state, lower_bound, head_gain):
    nseq, heads, width = (state.shape[0], state.shape[1], state.shape[2])
    query = projected[:, 0].astype(jnp.float32).reshape(nseq, heads, width)
    forget_in = projected[:, 1].astype(jnp.float32)
    value = projected[:, 2].astype(jnp.float32).reshape(nseq, heads, width)
    outgate = projected[:, 3].astype(jnp.float32)
    forget = (lower_bound + (1.0 - lower_bound) * jax.nn.sigmoid(forget_in)).reshape(
        nseq, heads, width
    )
    keyed = ((1.0 - lower_bound) * jax.nn.sigmoid(-forget_in)).reshape(nseq, heads, width)
    fresh = forget[..., None] * state + keyed[..., None] * value[:, :, None, :]
    read = jnp.einsum("bhkv,bhk->bhv", fresh, query, precision=lax.Precision.HIGHEST)
    scaled = (
        read * lax.rsqrt(jnp.mean(jnp.square(read), axis=-1, keepdims=True) + HEAD_EPS) * head_gain
    )
    mixed = (scaled.reshape(nseq, heads * width) * jax.nn.silu(outgate)).astype(jnp.bfloat16)
    return (mixed, fresh)


def greet(n, me):
    barrier = pltpu.get_barrier_semaphore()

    @pl.loop(1, n)
    def _(k):
        pl.semaphore_signal(
            barrier, inc=1, device_id=(lax.rem(me + k, n),), device_id_type=MESH
        )

    pl.semaphore_wait(barrier, n - 1)


def start_all(source, dest, send_sem, recv_sem, n, me):
    @pl.loop(1, n)
    def _(k):
        peer = lax.rem(me + k, n)
        pltpu.make_async_remote_copy(
            src_ref=source(peer),
            dst_ref=dest.at[me],
            send_sem=send_sem.at[k],
            recv_sem=recv_sem.at[k],
            device_id=(peer,),
            device_id_type=MESH,
        ).start()


def wait_all(source, dest, send_sem, recv_sem, n, me):
    @pl.loop(1, n)
    def _(k):
        peer = lax.rem(me + k, n)
        pltpu.make_async_remote_copy(
            src_ref=source(peer),
            dst_ref=dest.at[lax.rem(me + n - k, n)],
            send_sem=send_sem.at[k],
            recv_sem=recv_sem.at[k],
            device_id=(peer,),
            device_id_type=MESH,
        ).wait()


def gather_all(block_ref, gathered, send_sem, recv_sem, n, me):
    chips = n // 2
    chip, core = lax.div(me, 2), lax.rem(me, 2)
    sibling = 2 * chip + 1 - core

    def across(k, owner):
        return pltpu.make_async_remote_copy(
            src_ref=block_ref,
            dst_ref=gathered.at[owner],
            send_sem=send_sem.at[k],
            recv_sem=recv_sem.at[k],
            device_id=(2 * lax.rem(chip + k, chips) + core,),
            device_id_type=MESH,
        )

    def onward(k, source, owner):
        return pltpu.make_async_remote_copy(
            src_ref=source,
            dst_ref=gathered.at[owner],
            send_sem=send_sem.at[chips + k],
            recv_sem=recv_sem.at[chips + k],
            device_id=(sibling,),
            device_id_type=MESH,
        )

    pl.loop(1, chips)(lambda k: across(k, me).start())
    onward(0, block_ref, me).start()
    gathered[me] = block_ref[...]

    @pl.loop(1, chips)
    def _(k):
        owner = 2 * lax.rem(chip + chips - k, chips) + core
        across(k, owner).wait()
        onward(k, gathered.at[owner], owner).start()

    onward(0, block_ref, sibling).wait()

    @pl.loop(1, chips)
    def _(k):
        base = 2 * lax.rem(chip + chips - k, chips)
        onward(k, gathered.at[base + core], base + 1 - core).wait()


def dot_turned(rows, weight):
    return lax.dot_general(
        rows, weight, (((1,), (1,)), ((), ())), preferred_element_type=jnp.float32
    )


def flatten_rows(blocks, flat, n, nseq):
    group = max(1, 16 // nseq)

    @pl.loop(0, n // group)
    def _(i):
        parts = [blocks[i * group + j].astype(jnp.float32) for j in range(group)]
        at = pl.multiple_of(i * (group * nseq), group * nseq)
        flat[pl.ds(at, group * nseq), :] = jnp.concatenate(parts, axis=0).astype(flat.dtype)


def split_rows(flat, blocks, n, nseq):
    group = max(1, 8 // nseq)

    @pl.loop(0, n // group)
    def _(i):
        at = pl.multiple_of(i * (group * nseq), group * nseq)
        taken = flat[pl.ds(at, group * nseq), :]
        for j in range(group):
            blocks[i * group + j] = taken[j * nseq : (j + 1) * nseq].astype(blocks.dtype)


def project_kernel(
    n, block_ref, weight_hbm, out_ref,
    weight, gathered, rows, made, outgoing, landed,
    weight_sem, gather_send, gather_recv, back_send, back_recv,
):
    me = lax.axis_index("ep")
    nseq = block_ref.shape[0]
    load = pltpu.make_async_copy(weight_hbm, weight, weight_sem)
    load.start()
    greet(n, me)
    gather_all(block_ref, gathered, gather_send, gather_recv, n, me)
    flatten_rows(gathered, rows, n, nseq)
    load.wait()
    made[...] = dot_turned(rows[...], weight[...])
    split_rows(made, outgoing, n, nseq)
    part = lambda peer: outgoing.at[peer]
    start_all(part, landed, back_send, back_recv, n, me)
    landed[me] = outgoing[me]
    wait_all(part, landed, back_send, back_recv, n, me)
    out_ref[...] = landed[...]


def exchange_semaphores(n):
    return [pltpu.SemaphoreType.DMA((n,))] * 4


def project(block, weight, n, collective_id):
    nseq, width = block.shape
    cols = weight.shape[0]
    bf16, f32 = jnp.bfloat16, jnp.float32
    return pl.pallas_call(
        functools.partial(project_kernel, n),
        out_shape=jax.ShapeDtypeStruct((n, nseq, cols), bf16),
        in_specs=[
            pl.BlockSpec(memory_space=pltpu.VMEM),
            pl.BlockSpec(memory_space=pl.ANY),
        ],
        out_specs=pl.BlockSpec(memory_space=pltpu.VMEM),
        scratch_shapes=[
            pltpu.VMEM(weight.shape, bf16),
            pltpu.VMEM((n, nseq, width), bf16),
            pltpu.VMEM((n * nseq, width), bf16),
            pltpu.VMEM((n * nseq, cols), f32),
            pltpu.VMEM((n, nseq, cols), bf16),
            pltpu.VMEM((n, nseq, cols), bf16),
            pltpu.SemaphoreType.DMA,
            *exchange_semaphores(n),
        ],
        compiler_params=pltpu.CompilerParams(
            collective_id=collective_id, has_side_effects=True, vmem_limit_bytes=24 * 2**20
        ),
    )(block, weight)


def column_tile(cols):
    return 256 if cols % 256 == 0 else cols


def for_tiles(cols, body):
    tile = column_tile(cols)
    if tile == cols:
        body(slice(None))
    else:
        pl.loop(0, cols // tile)(lambda i: body(pl.ds(pl.multiple_of(i * tile, tile), tile)))


def channel_kernel(
    n, block_ref, pick_ref, small_ref, gain_ref, bias_ref,
    gate_hbm, up_hbm, down_hbm, dense_gate_hbm, dense_up_hbm, dense_down_hbm, out_ref,
    gate_w, up_w, down_w, dense_gate_w, dense_up_w, dense_down_w,
    gathered, rows, hidden, dense_hidden, made, outgoing, landed,
    weight_sem, gather_send, gather_recv, back_send, back_recv,
):
    f32 = jnp.float32
    me = lax.axis_index("ep")
    nseq, width = block_ref.shape
    pairs = (
        (dense_gate_hbm, dense_gate_w),
        (dense_up_hbm, dense_up_w),
        (gate_hbm, gate_w),
        (up_hbm, up_w),
        (dense_down_hbm, dense_down_w),
        (down_hbm, down_w),
    )
    loads = [
        pltpu.make_async_copy(there, here, weight_sem.at[i]) for i, (there, here) in enumerate(pairs)
    ]
    for load in loads:
        load.start()
    greet(n, me)
    gather_all(block_ref, gathered, gather_send, gather_recv, n, me)
    flatten_rows(gathered, rows, n, nseq)
    dot = functools.partial(jnp.dot, preferred_element_type=f32)

    small = dot_turned(rows[...], small_ref[...])
    picks = pick_ref[...]
    logit_gap = jnp.sum(small[:, :EXPERTS] * picks[:, :EXPERTS], axis=1, keepdims=True)
    share = jax.nn.sigmoid(logit_gap)
    branch_gate = jax.nn.sigmoid(small[:, EXPERTS : EXPERTS + 1])
    on_first = picks[:, EXPERTS : EXPERTS + 1] > 0
    on_second = picks[:, EXPERTS + 1 : EXPERTS + 2] > 0
    weight = jnp.where(on_first, share, jnp.where(on_second, 1.0 - share, 0.0))

    def fill(target, gate, up):
        def body(at):
            gate_part = dot(rows[...], gate[:, at])
            up_part = dot(rows[...], up[:, at])
            target[:, at] = (jax.nn.silu(gate_part) * up_part).astype(jnp.bfloat16)

        for_tiles(target.shape[1], body)

    for load in loads[:2]:
        load.wait()
    gate_part = dot_turned(rows[...], dense_gate_w[...])
    up_part = dot_turned(rows[...], dense_up_w[...])
    dense_hidden[...] = (jax.nn.silu(gate_part) * up_part).astype(jnp.bfloat16)
    for load in loads[2:4]:
        load.wait()
    fill(hidden, gate_w, up_w)
    for load in loads[4:]:
        load.wait()

    def down(at):
        routed = dot(hidden[...], down_w[:, at])
        dense = dot(dense_hidden[...], dense_down_w[:, at])
        made[:, at] = branch_gate * dense + jnp.where(weight > 0, weight * routed, 0.0)

    for_tiles(width, down)
    split_rows(made, outgoing, n, nseq)
    part = lambda peer: outgoing.at[peer]
    start_all(part, landed, back_send, back_recv, n, me)
    landed[me] = outgoing[me]
    wait_all(part, landed, back_send, back_recv, n, me)
    channel = lax.fori_loop(
        0, n, lambda d, total: total + landed[d].astype(f32), jnp.zeros((nseq, width), f32)
    )
    mixture = ALPHA * block_ref[...].astype(f32) + channel
    out_ref[...] = layer_norm(mixture, gain_ref[...], bias_ref[...]).astype(jnp.bfloat16)


def channel_and_norm(
    normed, routes, n, router_weight, branch_vector, dense_gate_weight, dense_up_weight,
    dense_down_weight, expert_gate_weight, expert_up_weight, expert_down_weight, gain, bias,
):
    bf16, f32 = jnp.bfloat16, jnp.float32
    nseq, width = normed.shape
    total = n * nseq
    expert = lax.axis_index("ep") // (n // EXPERTS)
    first = jax.nn.one_hot(routes[:, 0], EXPERTS, dtype=f32)
    second = jax.nn.one_hot(routes[:, 1], EXPERTS, dtype=f32)
    picks = jnp.concatenate([first - second, (routes == expert).astype(f32)], axis=1)
    small = jnp.concatenate([router_weight.T, branch_vector[None]], axis=0)
    weights = (
        expert_gate_weight,
        expert_up_weight,
        expert_down_weight,
        dense_gate_weight.T,
        dense_up_weight.T,
        dense_down_weight,
    )
    vmem, anywhere = pl.BlockSpec(memory_space=pltpu.VMEM), pl.BlockSpec(memory_space=pl.ANY)
    return pl.pallas_call(
        functools.partial(channel_kernel, n),
        out_shape=jax.ShapeDtypeStruct((nseq, width), bf16),
        in_specs=[vmem] * 5 + [anywhere] * 6,
        out_specs=vmem,
        scratch_shapes=[
            *[pltpu.VMEM(w.shape, bf16) for w in weights],
            pltpu.VMEM((n, nseq, width), bf16),
            pltpu.VMEM((total, width), bf16),
            pltpu.VMEM((total, expert_gate_weight.shape[1]), bf16),
            pltpu.VMEM((total, dense_gate_weight.shape[1]), bf16),
            pltpu.VMEM((total, width), f32),
            pltpu.VMEM((n, nseq, width), bf16),
            pltpu.VMEM((n, nseq, width), bf16),
            pltpu.SemaphoreType.DMA((6,)),
            *exchange_semaphores(n),
        ],
        compiler_params=pltpu.CompilerParams(
            collective_id=2, has_side_effects=True, vmem_limit_bytes=56 * 2**20
        ),
    )(normed, picks, small, gain[None], bias[None], *weights)


def per_device(
    tokens,
    recurrent_state,
    query_weight,
    forget_weight,
    input_weight,
    outgate_weight,
    lower_bound,
    head_gain,
    mixout_weight,
    first_gain,
    first_bias,
    router_weight,
    branch_vector,
    dense_gate_weight,
    dense_up_weight,
    dense_down_weight,
    expert_gate_weight,
    expert_up_weight,
    expert_down_weight,
    second_gain,
    second_bias,
    routes,
):
    f32 = jnp.float32
    devices = lax.axis_size("ep")
    nseq, width = tokens.shape
    own_cols = query_weight.shape[1]
    stacked = jnp.concatenate(
        [query_weight.T, forget_weight.T, input_weight.T, outgate_weight.T], axis=0
    )
    owned = project(tokens, stacked, devices, 0)
    projected = (
        owned.reshape(devices, nseq, 4, own_cols)
        .transpose(1, 2, 0, 3)
        .reshape(nseq, 4, devices * own_cols)
    )
    mixed, new_state = recurrence(projected, recurrent_state, lower_bound, head_gain)
    mix_out = project(mixed, mixout_weight.T, devices, 1).transpose(1, 0, 2).reshape(nseq, width)
    normed = layer_norm(
        ALPHA * tokens.astype(f32) + mix_out.astype(f32), first_gain, first_bias
    ).astype(jnp.bfloat16)
    output = channel_and_norm(
        normed,
        routes,
        devices,
        router_weight,
        branch_vector,
        dense_gate_weight,
        dense_up_weight,
        dense_down_weight,
        expert_gate_weight,
        expert_up_weight,
        expert_down_weight,
        second_gain,
        second_bias,
    )
    return (output, new_state)


def solution(mesh):
    return jax.shard_map(
        per_device,
        mesh=mesh,
        in_specs=(
            P("ep", None),
            P("ep", None, None, None),
            P(None, "ep"),
            P(None, "ep"),
            P(None, "ep"),
            P(None, "ep"),
            P(),
            P(),
            P(None, "ep"),
            P(),
            P(),
            P(),
            P(),
            P(None, "ep"),
            P(None, "ep"),
            P("ep", None),
            P(None, "ep"),
            P(None, "ep"),
            P("ep", None),
            P(),
            P(),
            P(),
        ),
        out_specs=(P("ep", None), P("ep", None, None, None)),
        check_vma=False,
    )
```
